32 devices in a mesh: sp: 8 (over z, x), tp: 4 (over y, core).
Axes of the slice: x: 2, y: 2, z: 4, core: 2. Of those that a mesh axis runs over, the one named last changes fastest.
Arguments:
- tokens: bfloat16 [6144, 4096], P('sp', 'tp'), may hold values from -12 to 12
- query_weight: bfloat16 [4096, 2048], P(None, 'tp'), may hold values from -0.09375 to 0.09375
- key_weight: bfloat16 [4096, 2048], P(None, 'tp'), may hold values from -0.09375 to 0.09375
- value_weight: bfloat16 [4096, 2048], P(None, 'tp'), may hold values from -0.09375 to 0.09375
- position_bias: float32 [16, 320], P('tp'), may hold values from -104 to 154
- out_grad: bfloat16 [6144, 2048], P('sp', 'tp'), may hold values from -6 to 6
Outputs:
- input_grad: bfloat16 [6144, 4096], P('sp', 'tp')
- query_weight_grad: float32 [4096, 2048], P('sp', 'tp')
- key_weight_grad: float32 [4096, 2048], P('sp', 'tp')
- value_weight_grad: float32 [4096, 2048], P('sp', 'tp')
- bias_grad: float32 [16, 320], P('tp')
The draws below stay inside these ranges and needn't reach their ends.
All inputs are finite; a program needn't handle non-finite values.
Results may differ from the reference program's by a relative error of at most 0.014.
Values may be sent and summed in bfloat16 or wider, within the bound.
No kernel may reach another device: no remote copies, remote signals or barrier semaphores. Data moves between devices by JAX's collectives and lax.ppermute only.
A program may use at most 128 MiB of HBM per device.

```python
import jax
import jax.numpy as jnp
import numpy as np
from jax import lax

WIDTH = 4096
HEADS = 16
HEAD_DIM = 128
SEGMENT = 64
PREVIOUS = 4
CLIP = 256
TOKENS = 6144
ATT_WIDTH = 2048
BIAS_LEN = 320
N_TP = 4


def draw_tokens(key, part):
    base = jax.random.normal(jax.random.fold_in(key, 11), (TOKENS, WIDTH), jnp.float32)
    base = jnp.clip(base, -6.0, 6.0)
    return base.astype(jnp.bfloat16)


def draw_position_bias(key, part):
    base = jax.random.normal(jax.random.fold_in(key, 21), (HEADS, BIAS_LEN), jnp.float32)
    base = jnp.clip(base, -4.0, 4.0)
    return base.astype(jnp.float32)


def shard_levels(rng, shape, split, smallest, top_value):
    level = 1.0
    for dim, blocks in split:
        heights = jax.random.uniform(jax.random.fold_in(jax.random.fold_in(rng, 6), dim), (blocks,), jnp.float32, smallest / len(split), top_value / len(split))
        level = level * jnp.repeat(jnp.exp(heights), shape[dim] // blocks).reshape((-1,) + (1,) * (len(shape) - 1 - dim))
    return level


def bell_draw(stream_key, extent, scale, most, shards=(), kind=jnp.bfloat16):
    values = scale * jax.random.normal(stream_key, extent, jnp.float32)
    if shards:
        values = values * shard_levels(stream_key, extent, shards, -0.22, 0.18)
    return jnp.clip(values, -most, most).astype(kind)


def setup_inputs(seed: int = 0) -> dict:
    arg_keys = jax.random.split(jax.random.key(seed), 7)
    tokens = draw_tokens(jax.random.fold_in(arg_keys[6], 71), 0)
    query_weight = bell_draw(arg_keys[1], (WIDTH, ATT_WIDTH), WIDTH ** -0.5, 0.09375, ((1, 4),))
    key_weight = bell_draw(arg_keys[2], (WIDTH, ATT_WIDTH), WIDTH ** -0.5, 0.09375, ((1, 4),))
    value_weight = bell_draw(arg_keys[3], (WIDTH, ATT_WIDTH), WIDTH ** -0.5, 0.09375, ((1, 4),))
    position_bias = draw_position_bias(jax.random.fold_in(arg_keys[6], 71), 0)
    out_grad = bell_draw(arg_keys[5], (TOKENS, ATT_WIDTH), 1.0, 6.0, ((0, 8), (1, 4)))
    return {"tokens": tokens, "query_weight": query_weight, "key_weight": key_weight, "value_weight": value_weight, "position_bias": position_bias, "out_grad": out_grad}


def bias_index(segment, reach, clip):
    query_pos = np.arange(segment)[:, None]
    band_pos = np.arange(reach + segment)[None, :]
    return (np.minimum(reach + query_pos - band_pos, clip) + segment - 1).astype(np.int32)


def fold_band(parts, count, head):
    shaped = parts.reshape(count, PREVIOUS + 1, SEGMENT, head)
    total = jnp.zeros((count + PREVIOUS, SEGMENT, head), jnp.float32)
    for band in range(PREVIOUS + 1):
        total = total.at[band:band + count].add(shaped[:, band])
    return total.reshape((count + PREVIOUS) * SEGMENT, head)


def head_grads(operands):
    query, keys, values, upstream, table = operands
    length, head = query.shape
    reach = PREVIOUS * SEGMENT
    count = length // SEGMENT
    factor = head ** -0.5
    padding = jnp.zeros((reach, head), keys.dtype)
    key_seg = jnp.concatenate([padding, keys]).reshape(count + PREVIOUS, SEGMENT, head)
    value_seg = jnp.concatenate([padding, values]).reshape(count + PREVIOUS, SEGMENT, head)
    key_band = jnp.stack([key_seg[band:band + count] for band in range(PREVIOUS + 1)], axis=1).reshape(count, reach + SEGMENT, head)
    value_band = jnp.stack([value_seg[band:band + count] for band in range(PREVIOUS + 1)], axis=1).reshape(count, reach + SEGMENT, head)
    query_seg = query.reshape(count, SEGMENT, head)
    grad_seg = upstream.reshape(count, SEGMENT, head)
    flat_index = bias_index(SEGMENT, reach, CLIP)
    bias = table[flat_index]
    scores = jnp.einsum('cqd,ckd->cqk', query_seg.astype(jnp.float32), key_band.astype(jnp.float32)) * factor + bias[None]
    key_pos = jnp.arange(count)[:, None] * SEGMENT - reach + jnp.arange(reach + SEGMENT)[None, :]
    valid = (key_pos >= 0)[:, None, :]
    masked = jnp.where(valid, scores, -jnp.inf)
    top = jnp.max(masked, axis=-1, keepdims=True)
    logsum = top + jnp.log(jnp.sum(jnp.exp(masked - top), axis=-1, keepdims=True))
    weights = jnp.exp(masked - logsum)
    weights_low = weights.astype(jnp.bfloat16)
    prob_grad = jnp.einsum('cqd,ckd->cqk', grad_seg.astype(jnp.float32), value_band.astype(jnp.float32))
    delta = jnp.sum(weights * prob_grad, axis=-1, keepdims=True)
    score_grad = weights * (prob_grad - delta)
    score_low = score_grad.astype(jnp.bfloat16)
    query_grad = (jnp.einsum('cqk,ckd->cqd', score_low.astype(jnp.float32), key_band.astype(jnp.float32)) * factor).reshape(length, head).astype(jnp.bfloat16)
    key_parts = jnp.einsum('cqk,cqd->ckd', score_low.astype(jnp.float32), query_seg.astype(jnp.float32)) * factor
    value_parts = jnp.einsum('cqk,cqd->ckd', weights_low.astype(jnp.float32), grad_seg.astype(jnp.float32))
    key_grad = fold_band(key_parts, count, head)[reach:].astype(jnp.bfloat16)
    value_grad = fold_band(value_parts, count, head)[reach:].astype(jnp.bfloat16)
    summed = jnp.sum(score_grad, axis=0).reshape(-1)
    table_grad = jnp.zeros((table.shape[0],), jnp.float32).at[flat_index.reshape(-1)].add(summed)
    return query_grad, key_grad, value_grad, table_grad


def reference(tokens, query_weight, key_weight, value_weight, position_bias, out_grad):
    query = jnp.dot(tokens, query_weight, preferred_element_type=jnp.float32).astype(jnp.bfloat16)
    keys = jnp.dot(tokens, key_weight, preferred_element_type=jnp.float32).astype(jnp.bfloat16)
    values = jnp.dot(tokens, value_weight, preferred_element_type=jnp.float32).astype(jnp.bfloat16)

    def by_head(array):
        return array.reshape(TOKENS, HEADS, HEAD_DIM).transpose(1, 0, 2)

    def by_token(array):
        return array.transpose(1, 0, 2).reshape(TOKENS, HEADS * HEAD_DIM)

    head_query, head_key, head_value, bias_grad = lax.map(head_grads, (by_head(query), by_head(keys), by_head(values), by_head(out_grad), position_bias))
    query_grad = by_token(head_query)
    key_grad = by_token(head_key)
    value_grad = by_token(head_value)
    tokens_t = tokens.T
    query_weight_grad = jnp.dot(tokens_t, query_grad, preferred_element_type=jnp.float32)
    key_weight_grad = jnp.dot(tokens_t, key_grad, preferred_element_type=jnp.float32)
    value_weight_grad = jnp.dot(tokens_t, value_grad, preferred_element_type=jnp.float32)
    group = HEADS * HEAD_DIM // N_TP
    total = jnp.zeros((TOKENS, WIDTH), jnp.float32)
    for number in range(N_TP):
        lower = number * group
        upper = lower + group
        term = jnp.dot(query_grad[:, lower:upper], query_weight[:, lower:upper].T, preferred_element_type=jnp.float32)
        term = term + jnp.dot(key_grad[:, lower:upper], key_weight[:, lower:upper].T, preferred_element_type=jnp.float32)
        term = term + jnp.dot(value_grad[:, lower:upper], value_weight[:, lower:upper].T, preferred_element_type=jnp.float32)
        rounded = lax.optimization_barrier(term.astype(jnp.bfloat16))
        total = total + rounded.astype(jnp.float32)
    input_grad = total.astype(jnp.bfloat16)
    return (input_grad, query_weight_grad, key_weight_grad, value_weight_grad, bias_grad)
```

```python
import jax
import jax.numpy as jnp
from jax import lax
from jax.experimental import pallas as pl
from jax.experimental.pallas import tpu as pltpu
from jax.sharding import PartitionSpec as P

SEGMENT = 64
PREVIOUS = 4
REACH = PREVIOUS * SEGMENT
SPAN = REACH + SEGMENT
ROWS = 2 * SEGMENT
KEYS = REACH + ROWS
LANES = KEYS


def from_behind(value, axis, steps):
    count = lax.axis_size(axis)
    leading, last = (max(0, -steps), min(count, count - steps))
    return lax.ppermute(value, axis, [(source, source + steps) for source in range(leading, last)])


def contract_rows(left, right):
    return lax.dot_general(
        left, right, (((0,), (0,)), ((), ())), preferred_element_type=jnp.float32
    )


def contract_cols(left, right):
    return lax.dot_general(
        left, right, (((1,), (1,)), ((), ())), preferred_element_type=jnp.float32
    )


def attention_kernel(
    first_ref, q_ref, k_ref, v_ref, pk_ref, pv_ref, g_ref, along_ref,
    dq_ref, dk_ref, dv_ref, hk_ref, hv_ref, diag_ref,
    kx, vx, dkx, dvx, acc, bias_t,
):
    length, head = q_ref.shape
    factor = head ** (-0.5)
    kx[:REACH] = pk_ref[...]
    kx[REACH:] = k_ref[...]
    vx[:REACH] = pv_ref[...]
    vx[REACH:] = v_ref[...]
    row = lax.broadcasted_iota(jnp.int32, (SEGMENT, LANES), 0)
    col = lax.broadcasted_iota(jnp.int32, (SEGMENT, LANES), 1)
    back = SEGMENT - 1 - row
    table = jnp.broadcast_to(along_ref[0], (SEGMENT, LANES))
    step = 1
    while step < SEGMENT:
        table = jnp.where((back & step) != 0, pltpu.roll(table, LANES - step, 1), table)
        step *= 2
    table = jnp.where(col < SPAN, table, -jnp.inf)
    bias_t[...] = jnp.concatenate([table, pltpu.roll(table, SEGMENT, 1)], axis=0).T
    acc[...] = jnp.zeros_like(acc)
    dkx[...] = jnp.zeros_like(dkx)
    dvx[...] = jnp.zeros_like(dvx)
    blind = first_ref[0] * REACH
    for start in range(0, length, ROWS):
        rows = pl.ds(start, ROWS)
        seen = pl.ds(start, KEYS)
        q = q_ref[rows, :]
        g = g_ref[rows, :]
        k = kx[seen, :]
        scores = contract_cols(k, q) * factor + bias_t[...]
        if start < REACH:
            place = lax.broadcasted_iota(jnp.int32, (KEYS, ROWS), 0) + start
            scores = jnp.where(place < blind, -jnp.inf, scores)
        prob_grad = contract_cols(vx[seen, :], g)
        top = jnp.max(scores, axis=0, keepdims=True)
        power = jnp.exp(scores - top)
        weights = power * (1.0 / jnp.sum(power, axis=0, keepdims=True))
        delta = jnp.sum(weights * prob_grad, axis=0, keepdims=True)
        score_grad = weights * (prob_grad - delta)
        acc[...] += score_grad
        weights_low = weights.astype(jnp.bfloat16)
        score_low = score_grad.astype(jnp.bfloat16)
        dvx[seen, :] += jnp.dot(weights_low, g, preferred_element_type=jnp.float32)
        dkx[seen, :] += jnp.dot(score_low, q, preferred_element_type=jnp.float32)
        dq_ref[rows, :] = (contract_rows(score_low, k) * factor).astype(jnp.bfloat16)
    hk_ref[...] = (dkx[:REACH] * factor).astype(jnp.bfloat16)
    hv_ref[...] = dvx[:REACH].astype(jnp.bfloat16)
    dk_ref[...] = dkx[REACH:] * factor
    dv_ref[...] = dvx[REACH:]
    both = acc[...].T
    skew = both[:SEGMENT] + pltpu.roll(both[SEGMENT:], LANES - SEGMENT, 1)
    step = 1
    while step < SEGMENT:
        skew = jnp.where((back & step) != 0, pltpu.roll(skew, step, 1), skew)
        step *= 2
    diag_ref[0] = jnp.sum(skew, axis=0, keepdims=True)


def attention(first, query, keys, values, prev_keys, prev_values, out_grad, table):
    length, width = query.shape
    heads = table.shape[0]
    head = width // heads
    along = jnp.concatenate(
        [
            jnp.broadcast_to(table[:, -1:], (heads, SEGMENT - 1)),
            table[:, ::-1],
            jnp.zeros((heads, LANES - SEGMENT + 1 - table.shape[1]), jnp.float32),
        ],
        axis=1,
    )[:, None, :]
    whole = pl.BlockSpec((length, head), lambda h: (0, h))
    edge = pl.BlockSpec((REACH, head), lambda h: (0, h))
    line = pl.BlockSpec((1, 1, LANES), lambda h: (h, 0, 0))
    flops = 2 * 5 * heads * length * KEYS * head
    outs = pl.pallas_call(
        attention_kernel,
        grid=(heads,),
        in_specs=[
            pl.BlockSpec(memory_space=pltpu.SMEM),
            whole, whole, whole, edge, edge, whole, line,
        ],
        out_specs=[whole, whole, whole, edge, edge, line],
        out_shape=[
            jax.ShapeDtypeStruct((length, width), jnp.bfloat16),
            jax.ShapeDtypeStruct((length, width), jnp.float32),
            jax.ShapeDtypeStruct((length, width), jnp.float32),
            jax.ShapeDtypeStruct((REACH, width), jnp.bfloat16),
            jax.ShapeDtypeStruct((REACH, width), jnp.bfloat16),
            jax.ShapeDtypeStruct((heads, 1, LANES), jnp.float32),
        ],
        scratch_shapes=[
            pltpu.VMEM((REACH + length, head), jnp.bfloat16),
            pltpu.VMEM((REACH + length, head), jnp.bfloat16),
            pltpu.VMEM((REACH + length, head), jnp.float32),
            pltpu.VMEM((REACH + length, head), jnp.float32),
            pltpu.VMEM((KEYS, ROWS), jnp.float32),
            pltpu.VMEM((KEYS, ROWS), jnp.float32),
        ],
        cost_estimate=pl.CostEstimate(
            flops=flops, bytes_accessed=12 * length * width, transcendentals=heads * length * KEYS
        ),
        compiler_params=pltpu.CompilerParams(vmem_limit_bytes=32 * 1024 * 1024),
        name="segment_attention",
    )(first, query, keys, values, prev_keys, prev_values, out_grad, along)
    diag = outs[-1][:, 0]
    size = table.shape[1]
    bias_grad = jnp.concatenate(
        [
            diag[:, SEGMENT : SEGMENT + size - 1][:, ::-1],
            jnp.sum(diag[:, :SEGMENT], axis=1, keepdims=True),
        ],
        axis=1,
    )
    return [*outs[:-1], bias_grad]


def shards(tokens, query_weight, key_weight, value_weight, position_bias, out_grad):
    whole = lax.all_gather(tokens, "tp", axis=1, tiled=True)
    length = whole.shape[0]
    cut = length - REACH

    def project(rows, weight):
        return jnp.dot(rows, weight, preferred_element_type=jnp.float32).astype(jnp.bfloat16)

    keys = project(whole, key_weight)
    values = project(whole, value_weight)
    prev_keys, prev_values = from_behind((keys[cut:], values[cut:]), "sp", 1)
    query = project(whole, query_weight)
    first = (lax.axis_index("sp") == 0).astype(jnp.int32).reshape(1)
    query_grad, key_own, value_own, key_back, value_back, bias_local = attention(
        first, query, keys, values, prev_keys, prev_values, out_grad, position_bias
    )
    back_keys, back_values = from_behind((key_back, value_back), "sp", -1)

    def join(own, back):
        return jnp.concatenate([own[:cut], own[cut:] + back.astype(jnp.float32)]).astype(
            jnp.bfloat16
        )

    def reduce_weight(grad):
        part = contract_rows(whole, grad).astype(jnp.bfloat16)
        return lax.psum_scatter(part, "sp", scatter_dimension=0, tiled=True).astype(jnp.float32)

    query_weight_grad = reduce_weight(query_grad)
    key_grad = join(key_own, back_keys)
    value_grad = join(value_own, back_values)
    key_weight_grad = reduce_weight(key_grad)
    value_weight_grad = reduce_weight(value_grad)
    input_part = (
        contract_cols(query_grad, query_weight)
        + contract_cols(key_grad, key_weight)
        + contract_cols(value_grad, value_weight)
    )
    input_grad = lax.psum_scatter(
        input_part.astype(jnp.bfloat16), "tp", scatter_dimension=1, tiled=True
    )
    bias_grad = lax.psum(bias_local, "sp")
    return input_grad, query_weight_grad, key_weight_grad, value_weight_grad, bias_grad


def solution(mesh):
    in_specs = (
        P("sp", "tp"),
        P(None, "tp"),
        P(None, "tp"),
        P(None, "tp"),
        P("tp", None),
        P("sp", "tp"),
    )
    out_specs = (P("sp", "tp"), P("sp", "tp"), P("sp", "tp"), P("sp", "tp"), P("tp", None))
    return jax.shard_map(shards, mesh=mesh, in_specs=in_specs, out_specs=out_specs, check_vma=False)
```

```python
import jax
import jax.numpy as jnp
from jax import lax
from jax.experimental import pallas as pl
from jax.experimental.pallas import tpu as pltpu
from jax.sharding import PartitionSpec as P

SEGMENT = 64
PREVIOUS = 4
REACH = PREVIOUS * SEGMENT
SPAN = REACH + SEGMENT
ROWS = 2 * SEGMENT
KEYS = REACH + ROWS
LANES = KEYS


def from_behind(value, axis, steps):
    count = lax.axis_size(axis)
    leading, last = (max(0, -steps), min(count, count - steps))
    return lax.ppermute(value, axis, [(source, source + steps) for source in range(leading, last)])


def contract_rows(left, right):
    return lax.dot_general(
        left, right, (((0,), (0,)), ((), ())), preferred_element_type=jnp.float32
    )


def contract_cols(left, right):
    return lax.dot_general(
        left, right, (((1,), (1,)), ((), ())), preferred_element_type=jnp.float32
    )


def attention_kernel(
    first_ref, q_ref, k_ref, v_ref, pk_ref, pv_ref, g_ref, along_ref,
    dq_ref, dk_ref, dv_ref, hk_ref, hv_ref, diag_ref,
    kx, vx, dkx, dvx, acc, bias_t,
):
    length, head = q_ref.shape
    factor = head ** (-0.5)
    kx[:REACH] = pk_ref[...]
    kx[REACH:] = k_ref[...]
    vx[:REACH] = pv_ref[...]
    vx[REACH:] = v_ref[...]
    row = lax.broadcasted_iota(jnp.int32, (SEGMENT, LANES), 0)
    col = lax.broadcasted_iota(jnp.int32, (SEGMENT, LANES), 1)
    back = SEGMENT - 1 - row
    table = jnp.broadcast_to(along_ref[0], (SEGMENT, LANES))
    step = 1
    while step < SEGMENT:
        table = jnp.where((back & step) != 0, pltpu.roll(table, LANES - step, 1), table)
        step *= 2
    table = jnp.where(col < SPAN, table, -jnp.inf)
    bias_t[...] = jnp.concatenate([table, pltpu.roll(table, SEGMENT, 1)], axis=0).T
    acc[...] = jnp.zeros_like(acc)
    dkx[...] = jnp.zeros_like(dkx)
    dvx[...] = jnp.zeros_like(dvx)
    blind = first_ref[0] * REACH
    for start in range(0, length, ROWS):
        rows = pl.ds(start, ROWS)
        seen = pl.ds(start, KEYS)
        q = q_ref[rows, :]
        g = g_ref[rows, :]
        k = kx[seen, :]
        scores = contract_cols(k, q) * factor + bias_t[...]
        if start < REACH:
            place = lax.broadcasted_iota(jnp.int32, (KEYS, ROWS), 0) + start
            scores = jnp.where(place < blind, -jnp.inf, scores)
        prob_grad = contract_cols(vx[seen, :], g)
        top = jnp.max(scores, axis=0, keepdims=True)
        power = jnp.exp(scores - top)
        weights = power * (1.0 / jnp.sum(power, axis=0, keepdims=True))
        delta = jnp.sum(weights * prob_grad, axis=0, keepdims=True)
        score_grad = weights * (prob_grad - delta)
        acc[...] += score_grad
        weights_low = weights.astype(jnp.bfloat16)
        score_low = score_grad.astype(jnp.bfloat16)
        dvx[seen, :] += jnp.dot(weights_low, g, preferred_element_type=jnp.float32)
        dkx[seen, :] += jnp.dot(score_low, q, preferred_element_type=jnp.float32)
        dq_ref[rows, :] = (contract_rows(score_low, k) * factor).astype(jnp.bfloat16)
    hk_ref[...] = (dkx[:REACH] * factor).astype(jnp.bfloat16)
    hv_ref[...] = dvx[:REACH].astype(jnp.bfloat16)
    dk_ref[...] = dkx[REACH:] * factor
    dv_ref[...] = dvx[REACH:]
    both = acc[...].T
    skew = both[:SEGMENT] + pltpu.roll(both[SEGMENT:], LANES - SEGMENT, 1)
    step = 1
    while step < SEGMENT:
        skew = jnp.where((back & step) != 0, pltpu.roll(skew, step, 1), skew)
        step *= 2
    diag_ref[0] = jnp.sum(skew, axis=0, keepdims=True)


def attention(first, query, keys, values, prev_keys, prev_values, out_grad, table):
    length, width = query.shape
    heads = table.shape[0]
    head = width // heads
    along = jnp.concatenate(
        [
            jnp.broadcast_to(table[:, -1:], (heads, SEGMENT - 1)),
            table[:, ::-1],
            jnp.zeros((heads, LANES - SEGMENT + 1 - table.shape[1]), jnp.float32),
        ],
        axis=1,
    )[:, None, :]
    whole = pl.BlockSpec((length, head), lambda h: (0, h))
    edge = pl.BlockSpec((REACH, head), lambda h: (0, h))
    line = pl.BlockSpec((1, 1, LANES), lambda h: (h, 0, 0))
    flops = 2 * 5 * heads * length * KEYS * head
    outs = pl.pallas_call(
        attention_kernel,
        grid=(heads,),
        in_specs=[
            pl.BlockSpec(memory_space=pltpu.SMEM),
            whole, whole, whole, edge, edge, whole, line,
        ],
        out_specs=[whole, whole, whole, edge, edge, line],
        out_shape=[
            jax.ShapeDtypeStruct((length, width), jnp.bfloat16),
            jax.ShapeDtypeStruct((length, width), jnp.float32),
            jax.ShapeDtypeStruct((length, width), jnp.float32),
            jax.ShapeDtypeStruct((REACH, width), jnp.bfloat16),
            jax.ShapeDtypeStruct((REACH, width), jnp.bfloat16),
            jax.ShapeDtypeStruct((heads, 1, LANES), jnp.float32),
        ],
        scratch_shapes=[
            pltpu.VMEM((REACH + length, head), jnp.bfloat16),
            pltpu.VMEM((REACH + length, head), jnp.bfloat16),
            pltpu.VMEM((REACH + length, head), jnp.float32),
            pltpu.VMEM((REACH + length, head), jnp.float32),
            pltpu.VMEM((KEYS, ROWS), jnp.float32),
            pltpu.VMEM((KEYS, ROWS), jnp.float32),
        ],
        cost_estimate=pl.CostEstimate(
            flops=flops, bytes_accessed=12 * length * width, transcendentals=heads * length * KEYS
        ),
        compiler_params=pltpu.CompilerParams(vmem_limit_bytes=32 * 1024 * 1024),
        name="segment_attention",
    )(first, query, keys, values, prev_keys, prev_values, out_grad, along)
    diag = outs[-1][:, 0]
    size = table.shape[1]
    bias_grad = jnp.concatenate(
        [
            diag[:, SEGMENT : SEGMENT + size - 1][:, ::-1],
            jnp.sum(diag[:, :SEGMENT], axis=1, keepdims=True),
        ],
        axis=1,
    )
    return [*outs[:-1], bias_grad]


def shards(tokens, query_weight, key_weight, value_weight, position_bias, out_grad):
    whole = lax.all_gather(tokens, "tp", axis=1, tiled=True)
    length = whole.shape[0]
    cut = length - REACH
    count = lax.axis_size("sp")
    block = whole.shape[1] // count
    side = lax.axis_index("sp") % 2
    partners = [(index, index ^ 1) for index in range(count)]
    groups = [list(range(start, count, 2)) for start in range(2)]

    def rows_of(array, which):
        cut_up = array.reshape(length, -1, 2, block)
        return jnp.where(which == 0, cut_up[:, :, 0], cut_up[:, :, 1]).reshape(length, -1)

    given = lax.ppermute(rows_of(tokens, 1 - side), "sp", partners)
    other = lax.all_gather(given, "tp", axis=1, tiled=True)
    paired = jnp.concatenate([rows_of(whole, side), other])

    def project(rows, weight):
        return jnp.dot(rows, weight, preferred_element_type=jnp.float32).astype(jnp.bfloat16)

    keys = project(whole, key_weight)
    values = project(whole, value_weight)
    prev_keys, prev_values = from_behind((keys[cut:], values[cut:]), "sp", 1)
    query = project(whole, query_weight)
    first = (lax.axis_index("sp") == 0).astype(jnp.int32).reshape(1)
    query_grad, key_own, value_own, key_back, value_back, bias_local = attention(
        first, query, keys, values, prev_keys, prev_values, out_grad, position_bias
    )
    back_keys, back_values = from_behind((key_back, value_back), "sp", -1)

    def join(own, back):
        return jnp.concatenate([own[:cut], own[cut:] + back.astype(jnp.float32)]).astype(
            jnp.bfloat16
        )

    def reduce_weight(grad):
        pair = jnp.concatenate([grad, lax.ppermute(grad, "sp", partners)])
        part = contract_rows(paired, pair).astype(jnp.bfloat16)
        return lax.psum_scatter(
            part, "sp", scatter_dimension=0, axis_index_groups=groups, tiled=True
        ).astype(jnp.float32)

    query_weight_grad = reduce_weight(query_grad)
    key_grad = join(key_own, back_keys)
    value_grad = join(value_own, back_values)
    key_weight_grad = reduce_weight(key_grad)
    value_weight_grad = reduce_weight(value_grad)
    input_part = (
        contract_cols(query_grad, query_weight)
        + contract_cols(key_grad, key_weight)
        + contract_cols(value_grad, value_weight)
    )
    input_grad = lax.psum_scatter(
        input_part.astype(jnp.bfloat16), "tp", scatter_dimension=1, tiled=True
    )
    bias_grad = lax.psum(bias_local, "sp")
    return input_grad, query_weight_grad, key_weight_grad, value_weight_grad, bias_grad


def solution(mesh):
    in_specs = (
        P("sp", "tp"),
        P(None, "tp"),
        P(None, "tp"),
        P(None, "tp"),
        P("tp", None),
        P("sp", "tp"),
    )
    out_specs = (P("sp", "tp"), P("sp", "tp"), P("sp", "tp"), P("sp", "tp"), P("tp", None))
    return jax.shard_map(shards, mesh=mesh, in_specs=in_specs, out_specs=out_specs, check_vma=False)
```
